32 devices in a mesh: sp: 8 (over z, y), tp: 4 (over x, core).
Axes of the slice: x: 2, y: 2, z: 4, core: 2. Of those that a mesh axis runs over, the one named last changes fastest.
Arguments:
- tokens: bfloat16 [2048, 2048], P(('sp', 'tp')), may hold values from -6 to 6
- norm_gain: float32 [2048], replicated, may hold values from 0.1 to 6, as said below
- query_weight: bfloat16 [2048, 16, 128], P(None, 'tp'), may hold values from -0.21875 to 0.21875
- key_weight: bfloat16 [2048, 4, 128], P(None, 'tp'), may hold values from -0.125 to 0.125
- value_weight: bfloat16 [2048, 4, 128], P(None, 'tp'), may hold values from -0.125 to 0.125
- mix_lambda: float32 [16], P('tp'), may hold values from 0.3 to 0.8
- head_gain: float32 [128], replicated, may hold values from 0.1 to 1.9
- pool_weight: bfloat16 [2048, 4, 512], P(None, 'tp'), may hold values from -0.125 to 0.125
- pool_mix: bfloat16 [4, 512, 512], P('tp'), may hold values from -0.25 to 0.25
- pool_scale: float32 [4, 512], P('tp'), may hold values from 0.1 to 1.9
- gate_weight: bfloat16 [2048, 2, 2048], P(None, None, 'tp'), may hold values from -0.125 to 0.125
- out_weight: bfloat16 [2048, 2048], P('tp'), may hold values from -0.125 to 0.125
Outputs:
- mixed: bfloat16 [2048, 2048], P(('sp', 'tp'))
- log_sums: float32 [2, 16, 2048], P(None, 'tp', 'sp')
The draws below stay inside these ranges and needn't reach their ends.
Inputs may be any that keep to these rules, and one draw needn't show every extreme that they name: `norm_gain`: positive.
All inputs are finite; a program needn't handle non-finite values.
Results may differ from the reference program's by a relative error of at most 0.013.
Values may be sent and summed in bfloat16 or wider, within the bound.
A program may use at most 128 MiB of HBM per device.

```python
import math
import jax
import jax.numpy as jnp
from jax import lax

D = 2048
HEADS = 16
HD = 64
DV = 128
KV_HEADS = 4
GROUPS = 4
GW = 512
WINDOW = 16
TOKENS = 2048
N_TP = 4


def draw_norm_gain(key, part):
    return 1.0 + 0.18 * jnp.clip(jax.random.normal(key, (D,), jnp.float32), -5.0, 5.0)


def block_levels(stream_key, extent, shards, least, largest):
    factor_of = 1.0
    for dim, parts in shards:
        draws = jax.random.uniform(jax.random.fold_in(jax.random.fold_in(stream_key, 6), dim), (parts,), jnp.float32, least / len(shards), largest / len(shards))
        factor_of = factor_of * jnp.repeat(jnp.exp(draws), extent[dim] // parts).reshape((-1,) + (1,) * (len(extent) - 1 - dim))
    return factor_of


def bell_draw(own_key, dims, width, most, cuts=(), held_as=jnp.bfloat16):
    values = width * jax.random.normal(own_key, dims, jnp.float32)
    if cuts:
        values = values * block_levels(own_key, dims, cuts, -0.22, 0.18)
    return jnp.clip(values, -most, most).astype(held_as)


def setup_inputs(seed: int = 0) -> dict:
    key_list = jax.random.split(jax.random.key(seed), 13)
    return {
        "tokens": bell_draw(key_list[0], (TOKENS, D), 1.0, 6.0, ((0, 32),)),
        "norm_gain": draw_norm_gain(jax.random.fold_in(key_list[12], 71), 0),
        "query_weight": bell_draw(key_list[2], (D, HEADS, 2 * HD), (D // 3) ** -0.5, 0.21875, ((1, 4),)),
        "key_weight": bell_draw(key_list[3], (D, KV_HEADS, 2 * HD), D ** -0.5, 0.125, ((1, 4),)),
        "value_weight": bell_draw(key_list[4], (D, KV_HEADS, DV), D ** -0.5, 0.125, ((1, 4),)),
        "mix_lambda": jnp.clip(0.3 + 0.5 * jax.random.uniform(key_list[5], (HEADS,), jnp.float32) ** block_levels(key_list[5], (HEADS,), ((0, 4),), -0.2, 0.2), 0.3, 0.8),
        "head_gain": jnp.clip(1.0 + 0.18 * jax.random.normal(key_list[6], (DV,), jnp.float32), 0.1, 1.9),
        "pool_weight": bell_draw(key_list[7], (D, GROUPS, GW), D ** -0.5, 0.125, ((1, 4),)),
        "pool_mix": bell_draw(key_list[8], (GROUPS, GW, GW), GW ** -0.5, 0.25, ((0, 4),)),
        "pool_scale": jnp.clip(1.0 + 0.18 * jax.random.normal(key_list[9], (GROUPS, GW), jnp.float32), 0.1, 1.9),
        "gate_weight": bell_draw(key_list[10], (D, 2, D), D ** -0.5, 0.125, ((2, 4),)),
        "out_weight": bell_draw(key_list[11], (D, D), D ** -0.5, 0.125, ((0, 4),)),
    }


NORM_EPS = 1e-06

def reference(tokens, norm_gain, query_weight, key_weight, value_weight, mix_lambda, head_gain, pool_weight, pool_mix, pool_scale, gate_weight, out_weight):
    inputs = tokens.astype(jnp.float32)
    normed = (inputs * lax.rsqrt(lax.optimization_barrier(jnp.mean(inputs * inputs, axis=1, keepdims=True)) + NORM_EPS) * norm_gain).astype(jnp.bfloat16)

    def project(weight):
        return jnp.dot(normed, weight.reshape(D, -1), preferred_element_type=jnp.float32).astype(jnp.bfloat16)
    queries = project(query_weight).reshape(TOKENS, HEADS, 2, HD)
    keys_all = project(key_weight).reshape(TOKENS, KV_HEADS, 2, HD)
    values_all = project(value_weight).reshape(TOKENS, KV_HEADS, DV)
    pool_in = project(pool_weight).reshape(TOKENS, GROUPS, GW)
    gate_pre = project(gate_weight).reshape(TOKENS, 2, D)
    group_size = HEADS // KV_HEADS
    block_rows = math.gcd(TOKENS, 1024)
    positions = jnp.arange(TOKENS, dtype=jnp.int32)
    score_scale = HD ** (-0.5)

    def one_head(head_index):
        kv_index = head_index // group_size
        head_queries = lax.dynamic_index_in_dim(queries, head_index, 1, keepdims=False).astype(jnp.float32)
        head_keys = lax.dynamic_index_in_dim(keys_all, kv_index, 1, keepdims=False).astype(jnp.float32)
        head_values = lax.dynamic_index_in_dim(values_all, kv_index, 1, keepdims=False)
        weight_lambda = lax.dynamic_index_in_dim(mix_lambda, head_index, 0, keepdims=False)

        def one_block(block_index):
            first_row = block_index * block_rows
            block_queries = lax.dynamic_slice_in_dim(head_queries, first_row, block_rows, 0)
            query_pos = first_row + jnp.arange(block_rows, dtype=jnp.int32)
            scores = jnp.einsum('qmd,kmd->mqk', block_queries, head_keys) * score_scale
            causal = positions[None, None, :] <= query_pos[None, :, None]
            masked = jnp.where(causal, scores, -jnp.inf)
            row_top = lax.optimization_barrier(jnp.max(masked, axis=2, keepdims=True))
            probs = jnp.exp(masked - row_top)
            row_sum = lax.optimization_barrier(jnp.sum(probs, axis=2, keepdims=True))
            log_total = row_top + jnp.log(row_sum)
            probs_low = probs.astype(jnp.bfloat16)
            first_map = jnp.dot(probs_low[0], head_values, preferred_element_type=jnp.float32)
            second_map = jnp.dot(probs_low[1], head_values, preferred_element_type=jnp.float32)
            block_out = first_map / row_sum[0] - weight_lambda * (second_map / row_sum[1])
            return (block_out, log_total[:, :, 0])
        outs, logs = lax.map(one_block, jnp.arange(TOKENS // block_rows, dtype=jnp.int32))
        return (outs.reshape(TOKENS, DV), jnp.transpose(logs, (1, 0, 2)).reshape(2, TOKENS))
    head_outs, head_logs = lax.map(one_head, jnp.arange(HEADS, dtype=jnp.int32))
    normed_heads = head_outs * lax.rsqrt(lax.optimization_barrier(jnp.mean(head_outs * head_outs, axis=2, keepdims=True)) + NORM_EPS) * head_gain
    attended = jnp.transpose(normed_heads, (1, 0, 2)).reshape(TOKENS, D)
    extended = jnp.concatenate([jnp.zeros((WINDOW, GROUPS, GW), jnp.float32), pool_in.astype(jnp.float32)], axis=0)
    group_parts = []
    for group_index in range(GROUPS):
        window_span = 2 ** (group_index + 1)
        window_sum = jnp.zeros((TOKENS, GW), jnp.float32)
        for back_rows in range(window_span):
            window_sum = window_sum + extended[WINDOW - back_rows:WINDOW - back_rows + TOKENS, group_index]
        counts = jnp.minimum(positions + 1, window_span).astype(jnp.float32)
        means = window_sum / counts[:, None]
        pooled = (means - pool_in[:, group_index].astype(jnp.float32)).astype(jnp.bfloat16)
        group_parts.append(jnp.dot(pooled, pool_mix[group_index], preferred_element_type=jnp.float32) * pool_scale[group_index])
    pool_out = jnp.concatenate(group_parts, axis=1)
    merged = (jax.nn.sigmoid(gate_pre[:, 0].astype(jnp.float32)) * attended + jax.nn.sigmoid(gate_pre[:, 1].astype(jnp.float32)) * pool_out).astype(jnp.bfloat16)
    block_cols = D // N_TP
    out_total = jnp.zeros((TOKENS, D), jnp.float32)
    for part_index in range(N_TP):
        partial_out = jnp.dot(merged[:, part_index * block_cols:(part_index + 1) * block_cols], out_weight[part_index * block_cols:(part_index + 1) * block_cols], preferred_element_type=jnp.float32).astype(jnp.bfloat16)
        out_total = out_total + lax.optimization_barrier(partial_out).astype(jnp.float32)
    return (out_total.astype(jnp.bfloat16), jnp.transpose(head_logs, (1, 0, 2)))
```

```python
import functools

import jax
import jax.numpy as jnp
from jax import lax
from jax.experimental import pallas as pl
from jax.experimental.pallas import tpu as pltpu
from jax.sharding import PartitionSpec as P

WINDOW = 16
NORM_EPS = 1e-06
MESH = pl.DeviceIdType.MESH
F32 = jnp.float32
BF16 = jnp.bfloat16
COLS = 256


def layer_kernel(
    S, T, heads, dims,
    lam_ref, tokens, gain_ref, wq_h, wk_h, wv_h, hgain_ref, wp_h, mix_h, pscale_ref, wg_h, wo_h,
    out_ref, lse_ref,
    tok, nrm, wkv, wq, wp, wg, wmix, wo, kvb, qt, acc, m_ref, l_ref, pool, gates, rim_out, rim_in,
    merged, part_remote, part_near, got_pair, got_near, sum_out, got_sum, keep,
    load_sem, tsend, trecv, ksend, krecv, rsem, psend, precv, ssend, srecv,
):
    R, HD, DV, GW, D = dims
    A = T // 2
    HALF = 2 * R
    rows = T * R
    QC = 2 * rows
    s = lax.axis_index("sp")
    t = lax.axis_index("tp")
    a = t // 2
    b = t % 2
    z = s // 2
    y = s % 2
    mate_t = 2 * a + 1 - b
    mate_s = 2 * z + 1 - y

    def slot(i):
        return pl.ds(pl.multiple_of(i * R, R), R)

    loads = [
        pltpu.make_async_copy(tokens, tok.at[slot(t)], load_sem.at[0]),
        pltpu.make_async_copy(wk_h, wkv.at[:, pl.ds(0, 2 * HD)], load_sem.at[1]),
        pltpu.make_async_copy(wv_h, wkv.at[:, pl.ds(2 * HD, DV)], load_sem.at[2]),
        pltpu.make_async_copy(wq_h, wq, load_sem.at[3]),
        pltpu.make_async_copy(wp_h, wp, load_sem.at[4]),
        pltpu.make_async_copy(wg_h, wg, load_sem.at[5]),
        pltpu.make_async_copy(mix_h, wmix, load_sem.at[6]),
        pltpu.make_async_copy(wo_h, wo, load_sem.at[7]),
    ]
    for load in loads:
        load.start()

    barrier = pltpu.get_barrier_semaphore()
    count = T - 1
    for d in range(1, T):
        pl.semaphore_signal(barrier, inc=1, device_id={"tp": (t + d) % T}, device_id_type=MESH)
    for d in (1, -1, 2, -2):
        ok = jnp.logical_and(s + d >= 0, s + d < S)

        @pl.when(ok)
        def _():
            pl.semaphore_signal(barrier, inc=1, device_id={"sp": s + d}, device_id_type=MESH)

        count = count + ok.astype(jnp.int32)
    pl.semaphore_wait(barrier, count)

    def tok_copy(i, lane, dst):
        return pltpu.make_async_remote_copy(
            src_ref=tok.at[slot(i)], dst_ref=tok.at[slot(i)],
            send_sem=tsend.at[lane], recv_sem=trecv.at[i],
            device_id={"tp": dst}, device_id_type=MESH)

    loads[0].wait()
    tok_sends = []
    for i in range(1, A):
        c = tok_copy(t, i, 2 * ((a + i) % A) + b)
        c.start()
        tok_sends.append(c)
    c = tok_copy(t, 0, mate_t)
    c.start()
    tok_sends.append(c)

    def kv_copy(j, p, lane, dst):
        return pltpu.make_async_remote_copy(
            src_ref=kvb.at[j, p], dst_ref=kvb.at[j, p],
            send_sem=ksend.at[(j * A + p) * 2 + lane], recv_sem=krecv.at[j * A + p],
            device_id={"sp": dst}, device_id_type=MESH)

    has_next = s + 2 < S

    def project_half(p):
        at = pl.ds(pl.multiple_of(p * HALF, HALF), HALF)
        x = tok[at].astype(F32)
        n = (x * lax.rsqrt(jnp.mean(x * x, axis=1, keepdims=True) + NORM_EPS) * gain_ref[...]).astype(BF16)
        nrm[at] = n
        kvb[s, p] = jnp.dot(n, wkv[...], preferred_element_type=F32).astype(BF16)

    def send_half(p):
        @pl.when(has_next)
        def _():
            kv_copy(s, p, 0, s + 2).start()

        @pl.when(y == 0)
        def _():
            kv_copy(s, p, 1, mate_s).start()

    tok_copy(mate_t, 0, mate_t).wait_recv()
    loads[1].wait()
    loads[2].wait()
    project_half(a)
    send_half(a)
    for i in range(1, A):
        far = (a + i) % A
        tok_copy(2 * far + b, 0, mate_t).wait_recv()
        c = tok_copy(2 * far + b, A - 1 + i, mate_t)
        c.start()
        tok_sends.append(c)
    for i in range(1, A):
        far = (a + i) % A
        tok_copy(2 * far + 1 - b, 0, mate_t).wait_recv()
        project_half(far)
        send_half(far)

    loads[3].wait()
    lane = lax.broadcasted_iota(jnp.int32, (rows, 2 * HD), 1)
    qscale = HD ** -0.5
    for h in range(heads):
        q = jnp.dot(nrm[...], wq[:, h * 2 * HD:(h + 1) * 2 * HD], preferred_element_type=F32)
        q = q.astype(BF16).astype(F32) * qscale
        qt[:, h * QC:h * QC + rows] = jnp.where(lane < HD, q, 0.0).T.astype(BF16)
        qt[:, h * QC + rows:(h + 1) * QC] = jnp.where(lane >= HD, q, 0.0).T.astype(BF16)

    loads[4].wait()
    for c0 in range(0, GW, COLS):
        pool[:, c0:c0 + COLS] = jnp.dot(nrm[...], wp[:, c0:c0 + COLS], preferred_element_type=F32).astype(BF16)
    rim_out[...] = pool[rows - WINDOW:, :]

    def rim_copy(dst):
        return pltpu.make_async_remote_copy(
            src_ref=rim_out, dst_ref=rim_in, send_sem=rsem.at[0], recv_sem=rsem.at[1],
            device_id={"sp": dst}, device_id_type=MESH)

    m_ref[...] = jnp.full_like(m_ref, -1e30)
    l_ref[...] = jnp.zeros_like(l_ref)
    acc[...] = jnp.zeros_like(acc)

    def attend(j, masked):
        blk = kvb[j].reshape(rows, 2 * HD + DV)
        keys = blk[:, :2 * HD]
        vt = blk[:, 2 * HD:].astype(F32).T.astype(BF16)
        if masked:
            ki = lax.broadcasted_iota(jnp.int32, (rows, QC), 0)
            qi = lax.broadcasted_iota(jnp.int32, (rows, QC), 1)
            qi = jnp.where(qi >= rows, qi - rows, qi)
            seen = ki <= qi
        for h in range(heads):
            cs = slice(h * QC, (h + 1) * QC)
            sc = jnp.dot(keys, qt[:, cs], preferred_element_type=F32)
            if masked:
                sc = jnp.where(seen, sc, -1e30)
            m_old = m_ref[:, cs]
            m_new = jnp.maximum(m_old, jnp.max(sc, axis=0, keepdims=True))
            p = jnp.exp(sc - m_new)
            if masked:
                p = jnp.where(seen, p, 0.0)
            alpha = jnp.exp(m_old - m_new)
            l_ref[:, cs] = l_ref[:, cs] * alpha + jnp.sum(p, axis=0, keepdims=True)
            acc[:, cs] = acc[:, cs] * alpha + jnp.dot(vt, p.astype(BF16), preferred_element_type=F32)
            m_ref[:, cs] = m_new

    @pl.when(s + 1 < S)
    def _():
        rim_copy(s + 1).start()

    attend(s, True)

    def chain(k, carry):
        j = 2 * (z - k) + y
        for p in range(A):
            kv_copy(j, p, 0, mate_s).wait_recv()

            @pl.when(has_next)
            def _():
                kv_copy(j, p, 0, s + 2).start()

            kv_copy(j, p, 1, mate_s).start()
        attend(j, False)
        return carry

    lax.fori_loop(1, z + 1, chain, 0)

    loads[5].wait()
    for c0 in range(0, 2 * GW, COLS):
        gates[:, c0:c0 + COLS] = jnp.dot(nrm[...], wg[:, c0:c0 + COLS], preferred_element_type=F32).astype(BF16)

    def mates(k, carry):
        j = 2 * (z - k) + 1 - y
        for p in range(A):
            kv_copy(j, p, 0, mate_s).wait_recv()
        attend(j, False)
        return carry

    @pl.when(s > 0)
    def _():
        rim_copy(s).wait_recv()

    @pl.when(s == 0)
    def _():
        rim_in[...] = jnp.zeros_like(rim_in)

    span = jnp.left_shift(jnp.int32(2), t)
    ri = lax.broadcasted_iota(jnp.int32, (rows, rows), 0)
    ci = lax.broadcasted_iota(jnp.int32, (rows, rows), 1)
    band = jnp.where(jnp.logical_and(ci <= ri, ci > ri - span), 1.0, 0.0).astype(BF16)
    ri2 = lax.broadcasted_iota(jnp.int32, (rows, WINDOW), 0)
    ci2 = lax.broadcasted_iota(jnp.int32, (rows, WINDOW), 1) - WINDOW
    band2 = jnp.where(ci2 > ri2 - span, 1.0, 0.0).astype(BF16)
    pos = s * rows + lax.broadcasted_iota(jnp.int32, (rows, 1), 0)
    counts = jnp.minimum(pos + 1, span).astype(F32)
    total = jnp.dot(band, pool[...], preferred_element_type=F32) + jnp.dot(
        band2, rim_in[...], preferred_element_type=F32)
    pooled = (total / counts - pool[...].astype(F32)).astype(BF16)
    loads[6].wait()
    pmixed = jnp.dot(pooled, wmix[...], preferred_element_type=F32) * pscale_ref[...]
    keep_pool = jax.nn.sigmoid(gates[:, GW:].astype(F32)) * pmixed
    keep[...] = keep_pool

    lax.fori_loop(1 - y, z + 1, mates, 0)

    for h in range(heads):
        c1 = slice(h * QC, h * QC + rows)
        c2 = slice(h * QC + rows, (h + 1) * QC)
        l1 = l_ref[:, c1]
        l2 = l_ref[:, c2]
        lse_ref[0, h:h + 1, :] = m_ref[:, c1] + jnp.log(l1)
        lse_ref[1, h:h + 1, :] = m_ref[:, c2] + jnp.log(l2)
        o = acc[:, c1] / l1 - lam_ref[h] * (acc[:, c2] / l2)
        o = o * lax.rsqrt(jnp.mean(o * o, axis=0, keepdims=True) + NORM_EPS)
        att = o.T * hgain_ref[...]
        hs = slice(h * DV, (h + 1) * DV)
        merged[:, hs] = (jax.nn.sigmoid(gates[:, hs].astype(F32)) * att + keep[:, hs]).astype(BF16)

    loads[7].wait()

    def product(i):
        return jnp.dot(merged[slot(i)], wo[...], preferred_element_type=F32)

    def pair_copy(i):
        return pltpu.make_async_remote_copy(
            src_ref=part_remote.at[i - 1], dst_ref=got_pair.at[i - 1],
            send_sem=psend.at[i], recv_sem=precv.at[i],
            device_id={"tp": mate_t}, device_id_type=MESH)

    near_copy = pltpu.make_async_remote_copy(
        src_ref=part_near, dst_ref=got_near, send_sem=psend.at[0], recv_sem=precv.at[0],
        device_id={"tp": mate_t}, device_id_type=MESH)

    def sum_copy(i):
        return pltpu.make_async_remote_copy(
            src_ref=sum_out.at[i - 1], dst_ref=got_sum.at[i - 1],
            send_sem=ssend.at[i], recv_sem=srecv.at[i],
            device_id={"tp": 2 * ((a + i) % A) + b}, device_id_type=MESH)

    for i in range(1, A):
        far = (a + i) % A
        part_remote[i - 1] = product(2 * far + 1 - b).astype(BF16)
        pair_copy(i).start()
    for i in range(1, A):
        far = (a + i) % A
        mine = product(2 * far + b)
        pair_copy(i).wait_recv()
        sum_out[i - 1] = (mine + got_pair[i - 1].astype(F32)).astype(BF16)
        sum_copy(i).start()
    part_near[...] = product(mate_t).astype(BF16)
    near_copy.start()
    result = product(t)
    near_copy.wait_recv()
    result = result + got_near[...].astype(F32)
    for i in range(1, A):
        sum_copy(i).wait_recv()
        result = result + got_sum[i - 1].astype(F32)
    out_ref[...] = result.astype(BF16)

    for c in tok_sends:
        c.wait_send()

    @pl.when(s + 1 < S)
    def _():
        rim_copy(s + 1).wait_send()

    def drain(k, carry):
        j = 2 * (z - k) + y
        for p in range(A):
            @pl.when(has_next)
            def _():
                kv_copy(j, p, 0, s + 2).wait_send()

            @pl.when(jnp.logical_or(k > 0, y == 0))
            def _():
                kv_copy(j, p, 1, mate_s).wait_send()
        return carry

    lax.fori_loop(0, z + 1, drain, 0)
    near_copy.wait_send()
    for i in range(1, A):
        pair_copy(i).wait_send()
        sum_copy(i).wait_send()


def local(
    tokens, norm_gain, query_weight, key_weight, value_weight, mix_lambda, head_gain,
    pool_weight, pool_mix, pool_scale, gate_weight, out_weight,
):
    S = lax.axis_size("sp")
    T = lax.axis_size("tp")
    A = T // 2
    R, D = tokens.shape
    heads = query_weight.shape[1]
    HD = query_weight.shape[2] // 2
    DV = value_weight.shape[2]
    GW = pool_weight.shape[2]
    rows = T * R
    kv_width = 2 * HD + DV
    columns = heads * 2 * rows
    assert key_weight.shape[1] == 1 and pool_weight.shape[1] == 1
    assert T % 2 == 0 and S % 2 == 0
    hbm = pl.BlockSpec(memory_space=pl.ANY)
    vmem = pl.BlockSpec(memory_space=pltpu.VMEM)
    smem = pl.BlockSpec(memory_space=pltpu.SMEM)
    dma = pltpu.SemaphoreType.DMA
    V = pltpu.VMEM
    return pl.pallas_call(
        functools.partial(layer_kernel, S, T, heads, (R, HD, DV, GW, D)),
        out_shape=(
            jax.ShapeDtypeStruct((R, D), BF16),
            jax.ShapeDtypeStruct((2, heads, rows), F32),
        ),
        in_specs=[smem, hbm, vmem, hbm, hbm, hbm, vmem, hbm, hbm, vmem, hbm, hbm],
        out_specs=(vmem, vmem),
        scratch_shapes=[
            V((rows, D), BF16), V((rows, D), BF16), V((D, kv_width), BF16),
            V((D, heads * 2 * HD), BF16), V((D, GW), BF16), V((D, 2 * GW), BF16),
            V((GW, GW), BF16), V((heads * DV, D), BF16),
            V((S, A, 2 * R, kv_width), BF16), V((2 * HD, columns), BF16), V((DV, columns), F32),
            V((1, columns), F32), V((1, columns), F32), V((rows, GW), BF16), V((rows, 2 * GW), BF16),
            V((WINDOW, GW), BF16), V((WINDOW, GW), BF16), V((rows, GW), BF16),
            V((A - 1, R, D), BF16), V((R, D), BF16), V((A - 1, R, D), BF16), V((R, D), BF16),
            V((A - 1, R, D), BF16), V((A - 1, R, D), BF16), V((rows, GW), F32),
            dma((8,)), dma((2 * A,)), dma((T,)), dma((S * A * 2,)), dma((S * A,)), dma((2,)),
            dma((A,)), dma((A,)), dma((A,)), dma((A,)),
        ],
        compiler_params=pltpu.CompilerParams(
            collective_id=0, has_side_effects=True, vmem_limit_bytes=60 * 1024 * 1024),
    )(
        mix_lambda, tokens, norm_gain.reshape(1, D), query_weight.reshape(D, -1),
        key_weight.reshape(D, -1), value_weight.reshape(D, -1), head_gain.reshape(1, DV),
        pool_weight.reshape(D, -1), pool_mix.reshape(GW, GW), pool_scale,
        gate_weight.reshape(D, -1), out_weight,
    )


def solution(mesh):
    in_specs = (
        P(("sp", "tp"), None), P(), P(None, "tp", None), P(None, "tp", None), P(None, "tp", None),
        P("tp"), P(), P(None, "tp", None), P("tp", None, None), P("tp", None),
        P(None, None, "tp"), P("tp", None),
    )
    out_specs = (P(("sp", "tp"), None), P(None, "tp", "sp"))
    return jax.shard_map(local, mesh=mesh, in_specs=in_specs, out_specs=out_specs, check_vma=False)
```

```python
import functools

import jax
import jax.numpy as jnp
from jax import lax
from jax.experimental import pallas as pl
from jax.experimental.pallas import tpu as pltpu
from jax.sharding import PartitionSpec as P

WINDOW = 16
NORM_EPS = 1e-06
MESH = pl.DeviceIdType.MESH
F32 = jnp.float32
BF16 = jnp.bfloat16
COLS = 256


def layer_kernel(
    S, T, heads, dims,
    lam_ref, tokens, gain_ref, wq_h, wk_h, wv_h, hgain_ref, wp_h, mix_h, pscale_ref, wg_h, wo_h,
    out_ref, lse_ref,
    tok, nrm, wkv, wq4, wq, wp, wg, x2, wmix, wo, kvb, qt, acc, m_ref, l_ref, pool, gates, rim_out, rim_in,
    merged, part_remote, part_near, got_pair, got_near, sum_out, got_sum, keep,
    load_sem, tsend, trecv, asend, ksend, krecv, rsem, psend, precv, ssend, srecv,
):
    R, HD, DV, GW, D = dims
    A = T // 2
    HALF = 2 * R
    rows = T * R
    QC = 2 * rows
    s = lax.axis_index("sp")
    t = lax.axis_index("tp")
    a = t // 2
    b = t % 2
    z = s // 2
    y = s % 2
    mate_t = 2 * a + 1 - b
    mate_s = 2 * z + 1 - y

    def slot(i):
        return pl.ds(pl.multiple_of(i * R, R), R)

    loads = [
        pltpu.make_async_copy(tokens, tok.at[slot(t)], load_sem.at[0]),
        pltpu.make_async_copy(wk_h, wkv.at[:, pl.ds(0, 2 * HD)], load_sem.at[1]),
        pltpu.make_async_copy(wv_h, wkv.at[:, pl.ds(2 * HD, DV)], load_sem.at[2]),
        pltpu.make_async_copy(wq_h, wq4, load_sem.at[3]),
        pltpu.make_async_copy(wp_h, wp, load_sem.at[4]),
        pltpu.make_async_copy(mix_h, wmix, load_sem.at[5]),
        pltpu.make_async_copy(wo_h, wo, load_sem.at[6]),
    ]
    gate_loads = [
        pltpu.make_async_copy(wg_h.at[:, c], wg.at[c], load_sem.at[7 + c]) for c in range(GW // 128)
    ]
    for load in loads[:4] + gate_loads + loads[4:]:
        load.start()

    barrier = pltpu.get_barrier_semaphore()
    count = T - 1
    for d in range(1, T):
        pl.semaphore_signal(barrier, inc=1, device_id={"tp": (t + d) % T}, device_id_type=MESH)

    def greet(zz, carry):
        @pl.when(zz != z)
        def _():
            pl.semaphore_signal(barrier, inc=1, device_id={"sp": 2 * zz + y}, device_id_type=MESH)

        return carry

    lax.fori_loop(0, S // 2, greet, 0)
    count = count + S // 2 - 1
    for d in (1, -1):
        ok = jnp.logical_and(s + d >= 0, s + d < S)

        @pl.when(ok)
        def _():
            pl.semaphore_signal(barrier, inc=1, device_id={"sp": s + d}, device_id_type=MESH)

        count = count + ok.astype(jnp.int32)
    pl.semaphore_wait(barrier, count)

    def tok_copy(i, lane, dst):
        return pltpu.make_async_remote_copy(
            src_ref=tok.at[slot(i)], dst_ref=tok.at[slot(i)],
            send_sem=tsend.at[lane], recv_sem=trecv.at[i],
            device_id={"tp": dst}, device_id_type=MESH)

    loads[0].wait()
    tok_sends = []
    for i in range(1, A):
        c = tok_copy(t, i, 2 * ((a + i) % A) + b)
        c.start()
        tok_sends.append(c)
    c = tok_copy(t, 0, mate_t)
    c.start()
    tok_sends.append(c)

    def kv_copy(j, p, lane, dst):
        return pltpu.make_async_remote_copy(
            src_ref=kvb.at[j, p], dst_ref=kvb.at[j, p],
            send_sem=ksend.at[(j * A + p) * 2 + lane], recv_sem=krecv.at[j * A + p],
            device_id={"sp": dst}, device_id_type=MESH)

    has_next = s + 2 < S

    def project_half(p):
        at = pl.ds(pl.multiple_of(p * HALF, HALF), HALF)
        x = tok[at].astype(F32)
        n = (x * lax.rsqrt(jnp.mean(x * x, axis=1, keepdims=True) + NORM_EPS) * gain_ref[...]).astype(BF16)
        nrm[at] = n
        kvb[s, p] = jnp.dot(n, wkv[...], preferred_element_type=F32).astype(BF16)

    def send_half(p):
        @pl.when(has_next)
        def _():
            kv_copy(s, p, 0, s + 2).start()

        @pl.when(y == 0)
        def _():
            kv_copy(s, p, 1, mate_s).start()

    def direct_copy(d):
        return pltpu.make_async_remote_copy(
            src_ref=kvb.at[s, a], dst_ref=kvb.at[s, a],
            send_sem=asend.at[d], recv_sem=krecv.at[s * A + a],
            device_id={"sp": s + 2 * d}, device_id_type=MESH)

    def send_direct(d, carry):
        direct_copy(d).start()
        return carry

    far_steps = S // 2 - z

    def gate_half(p):
        at = pl.ds(pl.multiple_of(p * HALF, HALF), HALF)
        er = lax.broadcasted_iota(jnp.int32, (128, 512), 0)
        ec = lax.broadcasted_iota(jnp.int32, (128, 512), 1)
        spread = jnp.where(ec == 2 * er + jnp.where(ec >= 256, 257, 0), 1.0, 0.0).astype(BF16)
        for k in range(D // 128):
            both = jnp.dot(nrm[at, k * 128:(k + 1) * 128], spread, preferred_element_type=F32).astype(BF16)
            x2[:HALF, k * 256:(k + 1) * 256] = both[:, :256]
            x2[HALF:, k * 256:(k + 1) * 256] = both[:, 256:]
        rows_of = wg.reshape(GW // 128, 2 * D, 128)
        for c in range(0, GW // 128, 2):
            w = jnp.concatenate([rows_of[c], rows_of[c + 1]], axis=1)
            r = jnp.dot(x2[...], w, preferred_element_type=F32).astype(BF16)
            gates[at, c * 128:c * 128 + 256] = r[:HALF]
            gates[at, GW + c * 128:GW + c * 128 + 256] = r[HALF:]

    tok_copy(mate_t, 0, mate_t).wait_recv()
    loads[1].wait()
    loads[2].wait()
    project_half(a)
    lax.fori_loop(1, far_steps, send_direct, 0)

    @pl.when(y == 0)
    def _():
        kv_copy(s, a, 1, mate_s).start()

    loads[3].wait()
    wq[...] = wq4[...].reshape(D, heads * 2 * HD)
    for load in gate_loads:
        load.wait()
    gate_half(a)
    for i in range(1, A):
        far = (a + i) % A
        tok_copy(2 * far + b, 0, mate_t).wait_recv()
        c = tok_copy(2 * far + b, A - 1 + i, mate_t)
        c.start()
        tok_sends.append(c)
    for i in range(1, A):
        far = (a + i) % A
        tok_copy(2 * far + 1 - b, 0, mate_t).wait_recv()
        project_half(far)
        send_half(far)

    def pass_near(k, carry):
        j = 2 * (z - k) + y
        kv_copy(j, a, 0, mate_s).wait_recv()
        kv_copy(j, a, 1, mate_s).start()
        return carry

    lax.fori_loop(1, z + 1, pass_near, 0)

    lane = lax.broadcasted_iota(jnp.int32, (rows, 2 * HD), 1)
    qscale = HD ** -0.5
    for h in range(heads):
        q = jnp.dot(nrm[...], wq[:, h * 2 * HD:(h + 1) * 2 * HD], preferred_element_type=F32)
        q = q.astype(BF16).astype(F32) * qscale
        qt[:, h * QC:h * QC + rows] = jnp.where(lane < HD, q, 0.0).T.astype(BF16)
        qt[:, h * QC + rows:(h + 1) * QC] = jnp.where(lane >= HD, q, 0.0).T.astype(BF16)

    loads[4].wait()
    for c0 in range(0, GW, COLS):
        pool[:, c0:c0 + COLS] = jnp.dot(nrm[...], wp[:, c0:c0 + COLS], preferred_element_type=F32).astype(BF16)
    rim_out[...] = pool[rows - WINDOW:, :]

    def rim_copy(dst):
        return pltpu.make_async_remote_copy(
            src_ref=rim_out, dst_ref=rim_in, send_sem=rsem.at[0], recv_sem=rsem.at[1],
            device_id={"sp": dst}, device_id_type=MESH)

    m_ref[...] = jnp.full_like(m_ref, -1e30)
    l_ref[...] = jnp.zeros_like(l_ref)
    acc[...] = jnp.zeros_like(acc)

    def attend(blk, masked):
        keys = blk[:, :2 * HD]
        vt = blk[:, 2 * HD:].astype(F32).T.astype(BF16)
        if masked:
            ki = lax.broadcasted_iota(jnp.int32, (rows, QC), 0)
            qi = lax.broadcasted_iota(jnp.int32, (rows, QC), 1)
            qi = jnp.where(qi >= rows, qi - rows, qi)
            seen = ki <= qi
        for h in range(heads):
            cs = slice(h * QC, (h + 1) * QC)
            sc = jnp.dot(keys, qt[:, cs], preferred_element_type=F32)
            if masked:
                sc = jnp.where(seen, sc, -1e30)
            m_old = m_ref[:, cs]
            m_new = jnp.maximum(m_old, jnp.max(sc, axis=0, keepdims=True))
            p = jnp.exp(sc - m_new)
            if masked:
                p = jnp.where(seen, p, 0.0)
            alpha = jnp.exp(m_old - m_new)
            l_ref[:, cs] = l_ref[:, cs] * alpha + jnp.sum(p, axis=0, keepdims=True)
            acc[:, cs] = acc[:, cs] * alpha + jnp.dot(vt, p.astype(BF16), preferred_element_type=F32)
            m_ref[:, cs] = m_new

    @pl.when(s + 1 < S)
    def _():
        rim_copy(s + 1).start()

    def whole(j):
        return kvb[j].reshape(rows, 2 * HD + DV)

    def pair(zz, p):
        return jnp.concatenate([kvb[2 * zz, p], kvb[2 * zz + 1, p]], axis=0)

    attend(whole(s), True)

    def chain(k, carry):
        j = 2 * (z - k) + y
        for i in range(1, A):
            p = (a + i) % A
            kv_copy(j, p, 0, mate_s).wait_recv()

            @pl.when(has_next)
            def _():
                kv_copy(j, p, 0, s + 2).start()

            kv_copy(j, p, 1, mate_s).start()
        kv_copy(2 * (z - k) + 1 - y, a, 0, mate_s).wait_recv()
        attend(pair(z - k, a), False)
        return carry

    lax.fori_loop(1, z + 1, chain, 0)

    @pl.when(y == 1)
    def _():
        for p in range(A):
            kv_copy(s - 1, p, 0, mate_s).wait_recv()
        attend(whole(s - 1), False)

    for i in range(1, A):
        gate_half((a + i) % A)

    def mates(k, carry):
        for i in range(1, A):
            p = (a + i) % A
            kv_copy(2 * (z - k) + 1 - y, p, 0, mate_s).wait_recv()
            attend(pair(z - k, p), False)
        return carry

    @pl.when(s > 0)
    def _():
        rim_copy(s).wait_recv()

    @pl.when(s == 0)
    def _():
        rim_in[...] = jnp.zeros_like(rim_in)

    span = jnp.left_shift(jnp.int32(2), t)
    ri = lax.broadcasted_iota(jnp.int32, (rows, rows), 0)
    ci = lax.broadcasted_iota(jnp.int32, (rows, rows), 1)
    band = jnp.where(jnp.logical_and(ci <= ri, ci > ri - span), 1.0, 0.0).astype(BF16)
    ri2 = lax.broadcasted_iota(jnp.int32, (rows, WINDOW), 0)
    ci2 = lax.broadcasted_iota(jnp.int32, (rows, WINDOW), 1) - WINDOW
    band2 = jnp.where(ci2 > ri2 - span, 1.0, 0.0).astype(BF16)
    pos = s * rows + lax.broadcasted_iota(jnp.int32, (rows, 1), 0)
    counts = jnp.minimum(pos + 1, span).astype(F32)
    total = jnp.dot(band, pool[...], preferred_element_type=F32) + jnp.dot(
        band2, rim_in[...], preferred_element_type=F32)
    pooled = (total / counts - pool[...].astype(F32)).astype(BF16)
    loads[5].wait()
    pmixed = jnp.dot(pooled, wmix[...], preferred_element_type=F32) * pscale_ref[...]
    keep_pool = jax.nn.sigmoid(gates[:, GW:].astype(F32)) * pmixed
    keep[...] = keep_pool

    lax.fori_loop(1, z + 1, mates, 0)

    for h in range(heads):
        c1 = slice(h * QC, h * QC + rows)
        c2 = slice(h * QC + rows, (h + 1) * QC)
        l1 = l_ref[:, c1]
        l2 = l_ref[:, c2]
        lse_ref[0, h:h + 1, :] = m_ref[:, c1] + jnp.log(l1)
        lse_ref[1, h:h + 1, :] = m_ref[:, c2] + jnp.log(l2)
        o = acc[:, c1] / l1 - lam_ref[h] * (acc[:, c2] / l2)
        o = o * lax.rsqrt(jnp.mean(o * o, axis=0, keepdims=True) + NORM_EPS)
        att = o.T * hgain_ref[...]
        hs = slice(h * DV, (h + 1) * DV)
        merged[:, hs] = (jax.nn.sigmoid(gates[:, hs].astype(F32)) * att + keep[:, hs]).astype(BF16)

    loads[6].wait()

    def product(i):
        return jnp.dot(merged[slot(i)], wo[...], preferred_element_type=F32)

    def pair_copy(i):
        return pltpu.make_async_remote_copy(
            src_ref=part_remote.at[i - 1], dst_ref=got_pair.at[i - 1],
            send_sem=psend.at[i], recv_sem=precv.at[i],
            device_id={"tp": mate_t}, device_id_type=MESH)

    near_copy = pltpu.make_async_remote_copy(
        src_ref=part_near, dst_ref=got_near, send_sem=psend.at[0], recv_sem=precv.at[0],
        device_id={"tp": mate_t}, device_id_type=MESH)

    def sum_copy(i):
        return pltpu.make_async_remote_copy(
            src_ref=sum_out.at[i - 1], dst_ref=got_sum.at[i - 1],
            send_sem=ssend.at[i], recv_sem=srecv.at[i],
            device_id={"tp": 2 * ((a + i) % A) + b}, device_id_type=MESH)

    for i in range(1, A):
        far = (a + i) % A
        part_remote[i - 1] = product(2 * far + 1 - b).astype(BF16)
        pair_copy(i).start()
    for i in range(1, A):
        far = (a + i) % A
        mine = product(2 * far + b)
        pair_copy(i).wait_recv()
        sum_out[i - 1] = (mine + got_pair[i - 1].astype(F32)).astype(BF16)
        sum_copy(i).start()
    part_near[...] = product(mate_t).astype(BF16)
    near_copy.start()
    result = product(t)
    near_copy.wait_recv()
    result = result + got_near[...].astype(F32)
    for i in range(1, A):
        sum_copy(i).wait_recv()
        result = result + got_sum[i - 1].astype(F32)
    out_ref[...] = result.astype(BF16)

    for c in tok_sends:
        c.wait_send()

    @pl.when(s + 1 < S)
    def _():
        rim_copy(s + 1).wait_send()

    def drain(k, carry):
        j = 2 * (z - k) + y
        for p in range(A):
            @pl.when(jnp.logical_and(has_next, p != a))
            def _():
                kv_copy(j, p, 0, s + 2).wait_send()

            @pl.when(jnp.logical_or(k > 0, y == 0))
            def _():
                kv_copy(j, p, 1, mate_s).wait_send()
        return carry

    lax.fori_loop(0, z + 1, drain, 0)

    def drain_direct(d, carry):
        direct_copy(d).wait_send()
        return carry

    lax.fori_loop(1, far_steps, drain_direct, 0)
    near_copy.wait_send()
    for i in range(1, A):
        pair_copy(i).wait_send()
        sum_copy(i).wait_send()


def hand_over(out_in, sums_in, out_ref, sums_ref):
    out_ref[...] = out_in[...]
    sums_ref[...] = sums_in[...]


def local(
    tokens, norm_gain, query_weight, key_weight, value_weight, mix_lambda, head_gain,
    pool_weight, pool_mix, pool_scale, gate_weight, out_weight,
):
    S = lax.axis_size("sp")
    T = lax.axis_size("tp")
    A = T // 2
    R, D = tokens.shape
    heads = query_weight.shape[1]
    HD = query_weight.shape[2] // 2
    DV = value_weight.shape[2]
    GW = pool_weight.shape[2]
    rows = T * R
    kv_width = 2 * HD + DV
    columns = heads * 2 * rows
    assert key_weight.shape[1] == 1 and pool_weight.shape[1] == 1
    assert T % 2 == 0 and S % 2 == 0
    hbm = pl.BlockSpec(memory_space=pl.ANY)
    vmem = pl.BlockSpec(memory_space=pltpu.VMEM)
    smem = pl.BlockSpec(memory_space=pltpu.SMEM)
    dma = pltpu.SemaphoreType.DMA
    V = pltpu.VMEM
    out, sums = pl.pallas_call(
        functools.partial(layer_kernel, S, T, heads, (R, HD, DV, GW, D)),
        out_shape=(
            jax.ShapeDtypeStruct((R, D), BF16),
            jax.ShapeDtypeStruct((2, heads, rows), F32),
        ),
        in_specs=[smem, hbm, vmem, hbm, hbm, hbm, vmem, hbm, hbm, vmem, hbm, hbm],
        out_specs=(vmem, vmem),
        scratch_shapes=[
            V((rows, D), BF16), V((rows, D), BF16), V((D, kv_width), BF16),
            V((D, heads, 2 * HD), BF16), V((D, heads * 2 * HD), BF16), V((D, GW), BF16),
            V((GW // 128, D, 2, 128), BF16), V((4 * R, 2 * D), BF16),
            V((GW, GW), BF16), V((heads * DV, D), BF16),
            V((S, A, 2 * R, kv_width), BF16), V((2 * HD, columns), BF16), V((DV, columns), F32),
            V((1, columns), F32), V((1, columns), F32), V((rows, GW), BF16), V((rows, 2 * GW), BF16),
            V((WINDOW, GW), BF16), V((WINDOW, GW), BF16), V((rows, GW), BF16),
            V((A - 1, R, D), BF16), V((R, D), BF16), V((A - 1, R, D), BF16), V((R, D), BF16),
            V((A - 1, R, D), BF16), V((A - 1, R, D), BF16), V((rows, GW), F32),
            dma((7 + GW // 128,)), dma((2 * A,)), dma((T,)), dma((S // 2,)), dma((S * A * 2,)), dma((S * A,)), dma((2,)),
            dma((A,)), dma((A,)), dma((A,)), dma((A,)),
        ],
        compiler_params=pltpu.CompilerParams(
            collective_id=0, has_side_effects=True, vmem_limit_bytes=60 * 1024 * 1024),
    )(
        mix_lambda, tokens, norm_gain.reshape(1, D), query_weight,
        key_weight.reshape(D, -1), value_weight.reshape(D, -1), head_gain.reshape(1, DV),
        pool_weight.reshape(D, -1), pool_mix.reshape(GW, GW), pool_scale,
        gate_weight.reshape(D, 2, GW // 128, 128).transpose(0, 2, 1, 3), out_weight,
    )
    return pl.pallas_call(
        hand_over,
        out_shape=(jax.ShapeDtypeStruct(out.shape, BF16), jax.ShapeDtypeStruct(sums.shape, F32)),
        in_specs=[vmem, vmem],
        out_specs=(vmem, vmem),
        compiler_params=pltpu.CompilerParams(vmem_limit_bytes=4 * 1024 * 1024),
    )(out, sums)


def solution(mesh):
    in_specs = (
        P(("sp", "tp"), None), P(), P(None, "tp", None), P(None, "tp", None), P(None, "tp", None),
        P("tp"), P(), P(None, "tp", None), P("tp", None, None), P("tp", None),
        P(None, None, "tp"), P("tp", None),
    )
    out_specs = (P(("sp", "tp"), None), P(None, "tp", "sp"))
    return jax.shard_map(local, mesh=mesh, in_specs=in_specs, out_specs=out_specs, check_vma=False)
```

```python
import functools

import jax
import jax.numpy as jnp
from jax import lax
from jax.experimental import pallas as pl
from jax.experimental.pallas import tpu as pltpu
from jax.sharding import PartitionSpec as P

WINDOW = 16
NORM_EPS = 1e-06
MESH = pl.DeviceIdType.MESH
F32 = jnp.float32
BF16 = jnp.bfloat16
COLS = 256


def layer_kernel(
    S, T, heads, dims,
    lam_ref, tokens, gain_ref, wq_h, wk_h, wv_h, hgain_ref, wp_h, mix_h, pscale_ref, wg_h, wo_h,
    out_ref, lse_ref,
    tok, nrm, wkv, wq4, wq, wp, wg, x2, wmix, wo, kvb, qt, acc, m_ref, l_ref, pool, gates, rim_out, rim_in,
    merged, part_remote, part_near, got_pair, got_near, sum_out, got_sum, keep,
    load_sem, tsend, trecv, asend, ksend, krecv, rsem, psend, precv, ssend, srecv,
):
    R, HD, DV, GW, D = dims
    A = T // 2
    HALF = 2 * R
    rows = T * R
    QC = 2 * rows
    s = lax.axis_index("sp")
    t = lax.axis_index("tp")
    a = t // 2
    b = t % 2
    z = s // 2
    y = s % 2
    mate_t = 2 * a + 1 - b
    mate_s = 2 * z + 1 - y

    def slot(i):
        return pl.ds(pl.multiple_of(i * R, R), R)

    loads = [
        pltpu.make_async_copy(tokens, tok.at[slot(t)], load_sem.at[0]),
        pltpu.make_async_copy(wk_h, wkv.at[:, pl.ds(0, 2 * HD)], load_sem.at[1]),
        pltpu.make_async_copy(wv_h, wkv.at[:, pl.ds(2 * HD, DV)], load_sem.at[2]),
        pltpu.make_async_copy(wq_h, wq4, load_sem.at[3]),
        pltpu.make_async_copy(wp_h, wp, load_sem.at[4]),
        pltpu.make_async_copy(mix_h, wmix, load_sem.at[5]),
        pltpu.make_async_copy(wo_h, wo, load_sem.at[6]),
    ]
    gate_loads = [
        pltpu.make_async_copy(wg_h.at[:, c], wg.at[c], load_sem.at[7 + c]) for c in range(GW // 128)
    ]
    for load in loads[:4] + gate_loads + loads[4:]:
        load.start()

    barrier = pltpu.get_barrier_semaphore()
    count = T - 1
    for d in range(1, T):
        pl.semaphore_signal(barrier, inc=1, device_id={"tp": (t + d) % T}, device_id_type=MESH)

    def greet(zz, carry):
        @pl.when(zz != z)
        def _():
            pl.semaphore_signal(barrier, inc=1, device_id={"sp": 2 * zz + y}, device_id_type=MESH)

        return carry

    lax.fori_loop(0, S // 2, greet, 0)
    count = count + S // 2 - 1
    for d in (1, -1):
        ok = jnp.logical_and(s + d >= 0, s + d < S)

        @pl.when(ok)
        def _():
            pl.semaphore_signal(barrier, inc=1, device_id={"sp": s + d}, device_id_type=MESH)

        count = count + ok.astype(jnp.int32)
    pl.semaphore_wait(barrier, count)

    def tok_copy(i, lane, dst):
        return pltpu.make_async_remote_copy(
            src_ref=tok.at[slot(i)], dst_ref=tok.at[slot(i)],
            send_sem=tsend.at[lane], recv_sem=trecv.at[i],
            device_id={"tp": dst}, device_id_type=MESH)

    loads[0].wait()
    tok_sends = []
    for i in range(1, A):
        c = tok_copy(t, i, 2 * ((a + i) % A) + b)
        c.start()
        tok_sends.append(c)
    c = tok_copy(t, 0, mate_t)
    c.start()
    tok_sends.append(c)

    def kv_copy(j, p, lane, dst):
        return pltpu.make_async_remote_copy(
            src_ref=kvb.at[j, p], dst_ref=kvb.at[j, p],
            send_sem=ksend.at[(j * A + p) * 2 + lane], recv_sem=krecv.at[j * A + p],
            device_id={"sp": dst}, device_id_type=MESH)

    has_next = s + 2 < S

    def project_half(p):
        at = pl.ds(pl.multiple_of(p * HALF, HALF), HALF)
        x = tok[at].astype(F32)
        n = (x * lax.rsqrt(jnp.mean(x * x, axis=1, keepdims=True) + NORM_EPS) * gain_ref[...]).astype(BF16)
        nrm[at] = n
        kvb[s, p] = jnp.dot(n, wkv[...], preferred_element_type=F32).astype(BF16)

    def send_half(p):
        @pl.when(has_next)
        def _():
            kv_copy(s, p, 0, s + 2).start()

        @pl.when(y == 0)
        def _():
            kv_copy(s, p, 1, mate_s).start()

    def direct_copy(d):
        return pltpu.make_async_remote_copy(
            src_ref=kvb.at[s, a], dst_ref=kvb.at[s, a],
            send_sem=asend.at[d], recv_sem=krecv.at[s * A + a],
            device_id={"sp": s + 2 * d}, device_id_type=MESH)

    def send_direct(d, carry):
        direct_copy(d).start()
        return carry

    far_steps = S // 2 - z

    def gate_half(p):
        at = pl.ds(pl.multiple_of(p * HALF, HALF), HALF)
        er = lax.broadcasted_iota(jnp.int32, (128, 512), 0)
        ec = lax.broadcasted_iota(jnp.int32, (128, 512), 1)
        spread = jnp.where(ec == 2 * er + jnp.where(ec >= 256, 257, 0), 1.0, 0.0).astype(BF16)
        for k in range(D // 128):
            both = jnp.dot(nrm[at, k * 128:(k + 1) * 128], spread, preferred_element_type=F32).astype(BF16)
            x2[:HALF, k * 256:(k + 1) * 256] = both[:, :256]
            x2[HALF:, k * 256:(k + 1) * 256] = both[:, 256:]
        rows_of = wg.reshape(GW // 128, 2 * D, 128)
        for c in range(0, GW // 128, 2):
            w = jnp.concatenate([rows_of[c], rows_of[c + 1]], axis=1)
            r = jnp.dot(x2[...], w, preferred_element_type=F32).astype(BF16)
            gates[at, c * 128:c * 128 + 256] = r[:HALF]
            gates[at, GW + c * 128:GW + c * 128 + 256] = r[HALF:]

    tok_copy(mate_t, 0, mate_t).wait_recv()
    loads[1].wait()
    loads[2].wait()
    project_half(a)
    lax.fori_loop(1, far_steps, send_direct, 0)

    @pl.when(y == 0)
    def _():
        kv_copy(s, a, 1, mate_s).start()

    loads[3].wait()
    wq[...] = wq4[...].reshape(D, heads * 2 * HD)
    for i in range(1, A):
        far = (a + i) % A
        tok_copy(2 * far + b, 0, mate_t).wait_recv()
        c = tok_copy(2 * far + b, A - 1 + i, mate_t)
        c.start()
        tok_sends.append(c)
    for i in range(1, A):
        far = (a + i) % A
        tok_copy(2 * far + 1 - b, 0, mate_t).wait_recv()
        project_half(far)
        send_half(far)

    def pass_near(k, carry):
        j = 2 * (z - k) + y
        kv_copy(j, a, 0, mate_s).wait_recv()
        kv_copy(j, a, 1, mate_s).start()
        return carry

    lax.fori_loop(1, z + 1, pass_near, 0)

    lane = lax.broadcasted_iota(jnp.int32, (rows, 2 * HD), 1)
    qscale = HD ** -0.5
    for h in range(heads):
        q = jnp.dot(nrm[...], wq[:, h * 2 * HD:(h + 1) * 2 * HD], preferred_element_type=F32)
        q = q.astype(BF16).astype(F32) * qscale
        qt[:, h * QC:h * QC + rows] = jnp.where(lane < HD, q, 0.0).T.astype(BF16)
        qt[:, h * QC + rows:(h + 1) * QC] = jnp.where(lane >= HD, q, 0.0).T.astype(BF16)

    loads[4].wait()
    for c0 in range(0, GW, COLS):
        pool[:, c0:c0 + COLS] = jnp.dot(nrm[...], wp[:, c0:c0 + COLS], preferred_element_type=F32).astype(BF16)
    rim_out[...] = pool[rows - WINDOW:, :]

    def rim_copy(dst):
        return pltpu.make_async_remote_copy(
            src_ref=rim_out, dst_ref=rim_in, send_sem=rsem.at[0], recv_sem=rsem.at[1],
            device_id={"sp": dst}, device_id_type=MESH)

    m_ref[...] = jnp.full_like(m_ref, -1e30)
    l_ref[...] = jnp.zeros_like(l_ref)
    acc[...] = jnp.zeros_like(acc)

    def attend(blk, masked):
        keys = blk[:, :2 * HD]
        vt = blk[:, 2 * HD:].astype(F32).T.astype(BF16)
        if masked:
            ki = lax.broadcasted_iota(jnp.int32, (rows, QC), 0)
            qi = lax.broadcasted_iota(jnp.int32, (rows, QC), 1)
            qi = jnp.where(qi >= rows, qi - rows, qi)
            seen = ki <= qi
        for h in range(heads):
            cs = slice(h * QC, (h + 1) * QC)
            sc = jnp.dot(keys, qt[:, cs], preferred_element_type=F32)
            if masked:
                sc = jnp.where(seen, sc, -1e30)
            m_old = m_ref[:, cs]
            m_new = jnp.maximum(m_old, jnp.max(sc, axis=0, keepdims=True))
            p = jnp.exp(sc - m_new)
            if masked:
                p = jnp.where(seen, p, 0.0)
            alpha = jnp.exp(m_old - m_new)
            l_ref[:, cs] = l_ref[:, cs] * alpha + jnp.sum(p, axis=0, keepdims=True)
            acc[:, cs] = acc[:, cs] * alpha + jnp.dot(vt, p.astype(BF16), preferred_element_type=F32)
            m_ref[:, cs] = m_new

    @pl.when(s + 1 < S)
    def _():
        rim_copy(s + 1).start()

    def whole(j):
        return kvb[j].reshape(rows, 2 * HD + DV)

    def pair(zz, p):
        return jnp.concatenate([kvb[2 * zz, p], kvb[2 * zz + 1, p]], axis=0)

    attend(whole(s), True)

    def chain(k, carry):
        j = 2 * (z - k) + y
        for i in range(1, A):
            p = (a + i) % A
            kv_copy(j, p, 0, mate_s).wait_recv()

            @pl.when(has_next)
            def _():
                kv_copy(j, p, 0, s + 2).start()

            kv_copy(j, p, 1, mate_s).start()
        kv_copy(2 * (z - k) + 1 - y, a, 0, mate_s).wait_recv()
        attend(pair(z - k, a), False)

        @pl.when(k <= A)
        def _():
            gate_half((a + k - 1) % A)

        return carry

    for load in gate_loads:
        load.wait()
    lax.fori_loop(1, z + 1, chain, 0)

    @pl.when(y == 1)
    def _():
        for p in range(A):
            kv_copy(s - 1, p, 0, mate_s).wait_recv()
        attend(whole(s - 1), False)

    def late_gates(k, carry):
        gate_half((a + k - 1) % A)
        return carry

    lax.fori_loop(jnp.minimum(z, A) + 1, A + 1, late_gates, 0)

    def mates(k, carry):
        for i in range(1, A):
            p = (a + i) % A
            kv_copy(2 * (z - k) + 1 - y, p, 0, mate_s).wait_recv()
            attend(pair(z - k, p), False)
        return carry

    @pl.when(s > 0)
    def _():
        rim_copy(s).wait_recv()

    @pl.when(s == 0)
    def _():
        rim_in[...] = jnp.zeros_like(rim_in)

    span = jnp.left_shift(jnp.int32(2), t)
    ri = lax.broadcasted_iota(jnp.int32, (rows, rows), 0)
    ci = lax.broadcasted_iota(jnp.int32, (rows, rows), 1)
    band = jnp.where(jnp.logical_and(ci <= ri, ci > ri - span), 1.0, 0.0).astype(BF16)
    ri2 = lax.broadcasted_iota(jnp.int32, (rows, WINDOW), 0)
    ci2 = lax.broadcasted_iota(jnp.int32, (rows, WINDOW), 1) - WINDOW
    band2 = jnp.where(ci2 > ri2 - span, 1.0, 0.0).astype(BF16)
    pos = s * rows + lax.broadcasted_iota(jnp.int32, (rows, 1), 0)
    counts = jnp.minimum(pos + 1, span).astype(F32)
    total = jnp.dot(band, pool[...], preferred_element_type=F32) + jnp.dot(
        band2, rim_in[...], preferred_element_type=F32)
    pooled = (total / counts - pool[...].astype(F32)).astype(BF16)
    loads[5].wait()
    pmixed = jnp.dot(pooled, wmix[...], preferred_element_type=F32) * pscale_ref[...]
    keep_pool = jax.nn.sigmoid(gates[:, GW:].astype(F32)) * pmixed
    keep[...] = keep_pool

    lax.fori_loop(1, z + 1, mates, 0)

    for h in range(heads):
        c1 = slice(h * QC, h * QC + rows)
        c2 = slice(h * QC + rows, (h + 1) * QC)
        l1 = l_ref[:, c1]
        l2 = l_ref[:, c2]
        lse_ref[0, h:h + 1, :] = m_ref[:, c1] + jnp.log(l1)
        lse_ref[1, h:h + 1, :] = m_ref[:, c2] + jnp.log(l2)
        o = acc[:, c1] / l1 - lam_ref[h] * (acc[:, c2] / l2)
        o = o * lax.rsqrt(jnp.mean(o * o, axis=0, keepdims=True) + NORM_EPS)
        att = o.T * hgain_ref[...]
        hs = slice(h * DV, (h + 1) * DV)
        merged[:, hs] = (jax.nn.sigmoid(gates[:, hs].astype(F32)) * att + keep[:, hs]).astype(BF16)

    loads[6].wait()

    def product(i):
        return jnp.dot(merged[slot(i)], wo[...], preferred_element_type=F32)

    def pair_copy(i):
        return pltpu.make_async_remote_copy(
            src_ref=part_remote.at[i - 1], dst_ref=got_pair.at[i - 1],
            send_sem=psend.at[i], recv_sem=precv.at[i],
            device_id={"tp": mate_t}, device_id_type=MESH)

    near_copy = pltpu.make_async_remote_copy(
        src_ref=part_near, dst_ref=got_near, send_sem=psend.at[0], recv_sem=precv.at[0],
        device_id={"tp": mate_t}, device_id_type=MESH)

    def sum_copy(i):
        return pltpu.make_async_remote_copy(
            src_ref=sum_out.at[i - 1], dst_ref=got_sum.at[i - 1],
            send_sem=ssend.at[i], recv_sem=srecv.at[i],
            device_id={"tp": 2 * ((a + i) % A) + b}, device_id_type=MESH)

    for i in range(1, A):
        far = (a + i) % A
        part_remote[i - 1] = product(2 * far + 1 - b).astype(BF16)
        pair_copy(i).start()
    for i in range(1, A):
        far = (a + i) % A
        mine = product(2 * far + b)
        pair_copy(i).wait_recv()
        sum_out[i - 1] = (mine + got_pair[i - 1].astype(F32)).astype(BF16)
        sum_copy(i).start()
    part_near[...] = product(mate_t).astype(BF16)
    near_copy.start()
    result = product(t)
    near_copy.wait_recv()
    result = result + got_near[...].astype(F32)
    for i in range(1, A):
        sum_copy(i).wait_recv()
        result = result + got_sum[i - 1].astype(F32)
    out_ref[...] = result.astype(BF16)

    for c in tok_sends:
        c.wait_send()

    @pl.when(s + 1 < S)
    def _():
        rim_copy(s + 1).wait_send()

    def drain(k, carry):
        j = 2 * (z - k) + y
        for p in range(A):
            @pl.when(jnp.logical_and(has_next, p != a))
            def _():
                kv_copy(j, p, 0, s + 2).wait_send()

            @pl.when(jnp.logical_or(k > 0, y == 0))
            def _():
                kv_copy(j, p, 1, mate_s).wait_send()
        return carry

    lax.fori_loop(0, z + 1, drain, 0)

    def drain_direct(d, carry):
        direct_copy(d).wait_send()
        return carry

    lax.fori_loop(1, far_steps, drain_direct, 0)
    near_copy.wait_send()
    for i in range(1, A):
        pair_copy(i).wait_send()
        sum_copy(i).wait_send()


def hand_over(out_in, sums_in, out_ref, sums_ref, sem):
    first = pltpu.make_async_copy(out_in, out_ref, sem.at[0])
    second = pltpu.make_async_copy(sums_in, sums_ref, sem.at[1])
    first.start()
    second.start()
    first.wait()
    second.wait()


def local(
    tokens, norm_gain, query_weight, key_weight, value_weight, mix_lambda, head_gain,
    pool_weight, pool_mix, pool_scale, gate_weight, out_weight,
):
    S = lax.axis_size("sp")
    T = lax.axis_size("tp")
    A = T // 2
    R, D = tokens.shape
    heads = query_weight.shape[1]
    HD = query_weight.shape[2] // 2
    DV = value_weight.shape[2]
    GW = pool_weight.shape[2]
    rows = T * R
    kv_width = 2 * HD + DV
    columns = heads * 2 * rows
    assert key_weight.shape[1] == 1 and pool_weight.shape[1] == 1
    assert T % 2 == 0 and S % 2 == 0
    hbm = pl.BlockSpec(memory_space=pl.ANY)
    vmem = pl.BlockSpec(memory_space=pltpu.VMEM)
    smem = pl.BlockSpec(memory_space=pltpu.SMEM)
    dma = pltpu.SemaphoreType.DMA
    V = pltpu.VMEM
    out, sums = pl.pallas_call(
        functools.partial(layer_kernel, S, T, heads, (R, HD, DV, GW, D)),
        out_shape=(
            jax.ShapeDtypeStruct((R, D), BF16),
            jax.ShapeDtypeStruct((2, heads, rows), F32),
        ),
        in_specs=[smem, hbm, vmem, hbm, hbm, hbm, vmem, hbm, hbm, vmem, hbm, hbm],
        out_specs=(vmem, vmem),
        scratch_shapes=[
            V((rows, D), BF16), V((rows, D), BF16), V((D, kv_width), BF16),
            V((D, heads, 2 * HD), BF16), V((D, heads * 2 * HD), BF16), V((D, GW), BF16),
            V((GW // 128, D, 2, 128), BF16), V((4 * R, 2 * D), BF16),
            V((GW, GW), BF16), V((heads * DV, D), BF16),
            V((S, A, 2 * R, kv_width), BF16), V((2 * HD, columns), BF16), V((DV, columns), F32),
            V((1, columns), F32), V((1, columns), F32), V((rows, GW), BF16), V((rows, 2 * GW), BF16),
            V((WINDOW, GW), BF16), V((WINDOW, GW), BF16), V((rows, GW), BF16),
            V((A - 1, R, D), BF16), V((R, D), BF16), V((A - 1, R, D), BF16), V((R, D), BF16),
            V((A - 1, R, D), BF16), V((A - 1, R, D), BF16), V((rows, GW), F32),
            dma((7 + GW // 128,)), dma((2 * A,)), dma((T,)), dma((S // 2,)), dma((S * A * 2,)), dma((S * A,)), dma((2,)),
            dma((A,)), dma((A,)), dma((A,)), dma((A,)),
        ],
        compiler_params=pltpu.CompilerParams(
            collective_id=0, has_side_effects=True, vmem_limit_bytes=60 * 1024 * 1024),
    )(
        mix_lambda, tokens, norm_gain.reshape(1, D), query_weight,
        key_weight.reshape(D, -1), value_weight.reshape(D, -1), head_gain.reshape(1, DV),
        pool_weight.reshape(D, -1), pool_mix.reshape(GW, GW), pool_scale,
        gate_weight.reshape(D, 2, GW // 128, 128).transpose(0, 2, 1, 3), out_weight,
    )
    return pl.pallas_call(
        hand_over,
        out_shape=(jax.ShapeDtypeStruct(out.shape, BF16), jax.ShapeDtypeStruct(sums.shape, F32)),
        in_specs=[hbm, hbm],
        out_specs=(vmem, vmem),
        scratch_shapes=[dma((2,))],
        compiler_params=pltpu.CompilerParams(vmem_limit_bytes=4 * 1024 * 1024),
    )(out, sums)


def solution(mesh):
    in_specs = (
        P(("sp", "tp"), None), P(), P(None, "tp", None), P(None, "tp", None), P(None, "tp", None),
        P("tp"), P(), P(None, "tp", None), P("tp", None, None), P("tp", None),
        P(None, None, "tp"), P("tp", None),
    )
    out_specs = (P(("sp", "tp"), None), P(None, "tp", "sp"))
    return jax.shard_map(local, mesh=mesh, in_specs=in_specs, out_specs=out_specs, check_vma=False)
```
